32 devices in a mesh: rep: 2 (over x), fs: 8 (over z, y), tp: 2 (over core).
Axes of the slice: x: 2, y: 2, z: 4, core: 2. Of those that a mesh axis runs over, the one named last changes fastest.
Arguments:
- states: bfloat16 [6144, 2048], P(('rep', 'fs'), 'tp'), may hold values from -6 to 6
- mix_gain: float32 [2048], replicated, may hold values from 0.1 to 1.9
- w_value: bfloat16 [2048, 2048], P('fs', 'tp'), may hold values from -1 to 1
- w_gate: bfloat16 [2048, 2048], P('fs', 'tp'), may hold values from -0.125 to 0.125
- conv_kernel: float32 [31, 2048], replicated, may hold values from -1 to 1
- chan_gain: float32 [2048], replicated, may hold values from 0.1 to 1.9
- w_mix_out: bfloat16 [2048, 2048], P('fs', 'tp'), may hold values from -0.125 to 0.125
- mlp_gain: float32 [2048], replicated, may hold values from 0.1 to 1.9
- w_up: bfloat16 [2048, 6144], P('fs', 'tp'), may hold values from -0.125 to 0.125
- w_down_t: bfloat16 [2048, 6144], P('fs', 'tp'), may hold values from -0.078125 to 0.078125
Outputs:
- layer_out: bfloat16 [6144, 2048], P(('rep', 'fs'), 'tp')
The draws below stay inside these ranges and needn't reach their ends.
All inputs are finite; a program needn't handle non-finite values.
Results may differ from the reference program's by a relative error of at most 0.017.
Values may be sent and summed in bfloat16 or wider, within the bound.
A program may use at most 64 MiB of HBM per device.

```python
import jax
import jax.numpy as jnp
from jax import lax

D = 2048
FF = 6144
KWIDTH = 31
LENGTH = 128
SEQS = 3
ROWS = 384
TOKENS = 6144
N_TP = 2


def draw_w_value(key, part):
    first_key, second_key = jax.random.split(jax.random.fold_in(key, 17))
    column = jnp.arange(D, dtype=jnp.float32)
    ramp = 10.0 ** (column / D)
    base = jnp.clip(jax.random.normal(first_key, (D, D), jnp.float32), -6.0, 6.0)
    jitter = jax.random.uniform(second_key, (D,), jnp.float32, 0.7, 1.3)
    scale = ramp * jitter / (3.0 * jnp.sqrt(jnp.float32(D)))
    return jnp.clip(base * scale[None, :], -1.0, 1.0).astype(jnp.bfloat16)


def shard_levels(own_key, shape, cuts, low, high):
    loudness, own = 1.0, jax.random.fold_in(own_key, 6)
    for position, blocks in cuts:
        heights = jnp.exp(jax.random.uniform(jax.random.fold_in(own, position), (blocks,), jnp.float32, low / len(cuts), high / len(cuts)))
        loudness = loudness * jnp.repeat(heights, shape[position] // blocks).reshape([-1 if axis == position else 1 for axis in range(len(shape))])
    return loudness


def normal_values(key, shape, deviation, most, cuts=(), kind=jnp.bfloat16):
    values = deviation * jax.random.normal(key, shape, jnp.float32)
    if cuts:
        values = values * shard_levels(key, shape, cuts, -0.22, 0.18)
    return jnp.clip(values, -most, most).astype(kind)


def setup_inputs(seed: int = 0) -> dict:
    arg_keys = jax.random.split(jax.random.key(seed), 11)
    return {
        "states": normal_values(arg_keys[0], (TOKENS, D), 1.0, 6.0, ((0, 16), (1, 2))),
        "mix_gain": jnp.clip(1.0 + 0.18 * jax.random.normal(arg_keys[1], (D,), jnp.float32), 0.1, 1.9),
        "w_value": draw_w_value(jax.random.fold_in(arg_keys[10], 71), 0),
        "w_gate": normal_values(arg_keys[3], (D, D), D ** -0.5, 0.125, ((0, 8), (1, 2))),
        "conv_kernel": normal_values(arg_keys[4], (KWIDTH, D), KWIDTH ** -0.5, 1.0, (), jnp.float32),
        "chan_gain": jnp.clip(1.0 + 0.18 * jax.random.normal(arg_keys[5], (D,), jnp.float32), 0.1, 1.9),
        "w_mix_out": normal_values(arg_keys[6], (D, D), D ** -0.5, 0.125, ((0, 8), (1, 2))),
        "mlp_gain": jnp.clip(1.0 + 0.18 * jax.random.normal(arg_keys[7], (D,), jnp.float32), 0.1, 1.9),
        "w_up": normal_values(arg_keys[8], (D, FF), D ** -0.5, 0.125, ((0, 8), (1, 2))),
        "w_down_t": normal_values(arg_keys[9], (D, FF), FF ** -0.5, 0.078125, ((0, 8), (1, 2))),
    }


EPS = 1e-06

def rms_norm(rows, gain):
    values = rows.astype(jnp.float32)
    scaled = values * lax.rsqrt(lax.optimization_barrier(jnp.mean(values * values, axis=-1, keepdims=True)) + EPS)
    return (scaled * gain).astype(jnp.bfloat16)

def causal_filter(gated, conv_kernel):
    width = gated.shape[1]
    blocks = gated.reshape(SEQS, LENGTH, width)
    padded = jnp.pad(blocks, ((0, 0), (KWIDTH - 1, 0), (0, 0)))
    total = jnp.zeros_like(blocks)
    for tap in range(KWIDTH):
        total = total + conv_kernel[tap][None, None, :] * padded[:, tap:tap + LENGTH, :]
    return total.reshape(SEQS * LENGTH, width)

def project_out(activated, weight_t):
    block = activated.shape[1] // N_TP
    total = jnp.zeros((activated.shape[0], weight_t.shape[0]), jnp.float32)
    for index in range(N_TP):
        piece = lax.dot_general(activated[:, index * block:(index + 1) * block], weight_t[:, index * block:(index + 1) * block], (((1,), (1,)), ((), ())), preferred_element_type=jnp.float32)
        total = total + piece.astype(jnp.bfloat16).astype(jnp.float32)
    return total

def one_group(rows, mix_gain, w_value, w_gate, conv_kernel, chan_gain, w_mix_out, mlp_gain, w_up, w_down_t):
    normed = rms_norm(rows, mix_gain)
    value = jnp.dot(normed, w_value, preferred_element_type=jnp.float32)
    gate = jnp.dot(normed, w_gate, preferred_element_type=jnp.float32)
    gated = value * jax.nn.sigmoid(gate)
    filtered = causal_filter(gated, conv_kernel)
    mean_rows = lax.optimization_barrier(jnp.mean(filtered, axis=-1, keepdims=True))
    variance = lax.optimization_barrier(jnp.mean(filtered * filtered, axis=-1, keepdims=True)) - mean_rows * mean_rows
    activated = jax.nn.silu((filtered - mean_rows) * lax.rsqrt(variance + EPS) * chan_gain).astype(jnp.bfloat16)
    middle = (rows.astype(jnp.float32) + project_out(activated, w_mix_out)).astype(jnp.bfloat16)
    normed_mid = rms_norm(middle, mlp_gain)
    upward = jnp.dot(normed_mid, w_up, preferred_element_type=jnp.float32)
    hidden = jnp.square(jnp.maximum(upward, 0.0)).astype(jnp.bfloat16)
    return (middle.astype(jnp.float32) + project_out(hidden, w_down_t)).astype(jnp.bfloat16)

def reference(states, mix_gain, w_value, w_gate, conv_kernel, chan_gain, w_mix_out, mlp_gain, w_up, w_down_t):
    groups = states.reshape(states.shape[0] // ROWS, ROWS, states.shape[1])

    def apply(rows):
        return one_group(rows, mix_gain, w_value, w_gate, conv_kernel, chan_gain, w_mix_out, mlp_gain, w_up, w_down_t)
    return lax.map(apply, groups).reshape(states.shape)
```

```python
import jax
import jax.numpy as jnp
from jax import lax
from jax.sharding import PartitionSpec as P

D = 2048
KWIDTH = 31
LENGTH = 128


EPS = 1e-06


def rms_norm(rows, gain):
    values = rows.astype(jnp.float32)
    scaled = values * lax.rsqrt(jnp.mean(values * values, axis=-1, keepdims=True) + EPS)
    return (scaled * gain).astype(jnp.bfloat16)


def times_transposed(left, right):
    return lax.dot_general(
        left, right, (((1,), (1,)), ((), ())), preferred_element_type=jnp.float32
    )


def body(
    states, mix_gain, w_value, w_gate, conv_kernel, chan_gain, w_mix_out, mlp_gain, w_up, w_down_t
):
    reps = lax.axis_size("rep")
    rep = lax.axis_index("rep")
    own_width = states.shape[1]
    width = own_width // reps
    offset = lax.axis_index("tp") * own_width + rep * width
    channels = own_width * lax.axis_size("tp")

    def own_columns(weight):
        part = weight.shape[1] // reps
        piece = lax.dynamic_slice_in_dim(weight, rep * part, part, 1)
        return lax.all_gather(piece, "fs", axis=0, tiled=True)

    def all_rows(rows):
        return lax.all_gather(
            lax.all_gather(rows, "tp", axis=1, tiled=True), "rep", axis=0, tiled=True
        )

    def own_sums(terms):
        terms = lax.psum_scatter(
            terms.astype(jnp.bfloat16), "rep", scatter_dimension=0, tiled=True
        )
        return lax.psum_scatter(terms, "tp", scatter_dimension=1, tiled=True).astype(jnp.float32)

    normed = rms_norm(all_rows(states), mix_gain)
    token_rows = normed.shape[0]
    value = jnp.dot(normed, own_columns(w_value), preferred_element_type=jnp.float32)
    gate = jnp.dot(normed, own_columns(w_gate), preferred_element_type=jnp.float32)
    gated = value * jax.nn.sigmoid(gate)
    own_kernel = lax.dynamic_slice_in_dim(conv_kernel, offset, width, 1)
    blocks = gated.reshape(token_rows // LENGTH, LENGTH, width)
    padded = jnp.pad(blocks, ((0, 0), (KWIDTH - 1, 0), (0, 0)))
    filtered = jnp.zeros_like(blocks)
    for tap in range(KWIDTH):
        filtered = filtered + own_kernel[tap][None, None, :] * padded[:, tap : tap + LENGTH, :]
    filtered = filtered.reshape(token_rows, width)
    sum_rows, square_rows = lax.psum(
        (jnp.sum(filtered, axis=-1), jnp.sum(filtered * filtered, axis=-1)), ("rep", "tp")
    )
    mean_rows = (sum_rows / channels)[:, None]
    variance = (square_rows / channels)[:, None] - mean_rows * mean_rows
    own_gain = lax.dynamic_slice_in_dim(chan_gain, offset, width, 0)
    activated = jax.nn.silu((filtered - mean_rows) * lax.rsqrt(variance + EPS) * own_gain).astype(
        jnp.bfloat16
    )
    mixed = own_sums(times_transposed(activated, own_columns(w_mix_out)))
    middle = (states.astype(jnp.float32) + mixed).astype(jnp.bfloat16)
    normed_mid = rms_norm(all_rows(middle), mlp_gain)
    upward = jnp.dot(normed_mid, own_columns(w_up), preferred_element_type=jnp.float32)
    hidden = jnp.square(jnp.maximum(upward, 0.0)).astype(jnp.bfloat16)
    fed = own_sums(times_transposed(hidden, own_columns(w_down_t)))
    return (middle.astype(jnp.float32) + fed).astype(jnp.bfloat16)


def solution(mesh):
    in_specs = (
        P(("rep", "fs"), "tp"),
        P(),
        P("fs", "tp"),
        P("fs", "tp"),
        P(),
        P(),
        P("fs", "tp"),
        P(),
        P("fs", "tp"),
        P("fs", "tp"),
    )
    out_specs = P(("rep", "fs"), "tp")
    return jax.shard_map(body, mesh=mesh, in_specs=in_specs, out_specs=out_specs, check_vma=False)
```

```python
import functools

import jax
import jax.numpy as jnp
from jax import lax
from jax.experimental import pallas as pl
from jax.experimental.pallas import tpu as pltpu
from jax.sharding import PartitionSpec as P

LENGTH = 128
LANES = 128
LEAD = 32
EPS = 1e-06
MESH = pl.DeviceIdType.MESH


def times_transposed(left, right):
    return lax.dot_general(
        left, right, (((1,), (1,)), ((), ())), preferred_element_type=jnp.float32
    )


def kernel(
    sizes,
    states, mix_gain, w_value, w_gate, conv_kernel, chan_gain, w_mix, mlp_gain, w_up, w_down,
    out,
    weights, rows_in, rows_mid, normed, padded, filtered, activated, hidden,
    own_stats, peer_stats, mix_parts, mix_peers, fed_parts, fed_peers,
    load_sems, ring_send, ring_recv, in_send, in_recv, mid_send, mid_recv,
    stat_send, stat_recv, mix_send, mix_recv, fed_send, fed_recv,
):
    reps, n, tps, rows, channels, width, ups = sizes
    own_width = width * reps
    half_way = n // 2
    shard = channels // n
    tokens = reps * rows
    pieces = tokens // LENGTH
    chunks = 3 + 2 * ups
    rep, fs, tp = lax.axis_index("rep"), lax.axis_index("fs"), lax.axis_index("tp")
    taps = conv_kernel.shape[0]
    blocks, _, block = mix_parts.shape
    per_tp = own_width // block

    def ring_index(place):
        place = lax.rem(place + n, n)
        return jnp.where(place < half_way, 2 * place, 2 * (n - 1 - place) + 1)

    place = jnp.where(lax.rem(fs, 2) == 0, fs // 2, n - 1 - fs // 2)
    neighbours = (ring_index(place + 1), ring_index(place - 1))

    barrier = pltpu.get_barrier_semaphore()
    for other in neighbours:
        pl.semaphore_signal(barrier, inc=1, device_id={"fs": other}, device_id_type=MESH)
    for dr in range(reps):
        for dt in range(tps):
            if dr or dt:
                pl.semaphore_signal(
                    barrier, inc=1,
                    device_id={"rep": lax.rem(rep + dr, reps), "tp": lax.rem(tp + dt, tps)},
                    device_id_type=MESH,
                )
    pl.semaphore_wait(barrier, 1 + reps * tps)

    own_rows = pl.ds(pl.multiple_of(rep * rows, rows), rows)
    own_cols = pl.ds(pl.multiple_of(tp * own_width, own_width), own_width)

    def shard_at(owner, start=0, size=None):
        size = shard if size is None else size
        return pl.ds(pl.multiple_of(owner * shard + start, size), size)

    def hop(c, s, way):
        sign = 1 if way == 0 else -1
        owner = ring_index(place - sign * (s - 1))
        span = shard_at(owner)
        if s == half_way:
            span = shard_at(owner, way * (shard // 2), shard // 2)
        return pltpu.make_async_remote_copy(
            src_ref=weights.at[c, span, :],
            dst_ref=weights.at[c, span, :],
            send_sem=ring_send.at[way, c],
            recv_sem=ring_recv.at[way, c, s - 1],
            device_id={"fs": neighbours[way]},
            device_id_type=MESH,
        )

    loads = []
    for c in range(chunks):
        if c < 3:
            source, column = (w_value, w_gate, w_mix)[c], rep * width
        elif c < 3 + ups:
            source, column = w_up, (rep * ups + c - 3) * width
        else:
            source, column = w_down, (rep * ups + c - 3 - ups) * width
        loads.append(
            pltpu.make_async_copy(
                source.at[:, pl.ds(pl.multiple_of(column, width), width)],
                weights.at[c, shard_at(fs), :],
                load_sems.at[c],
            )
        )
        loads[-1].start()
    own_load = pltpu.make_async_copy(states, rows_in.at[own_rows, own_cols], load_sems.at[chunks])
    own_load.start()

    def pump(c, s):
        for way in range(2):
            if s == 1:
                if way == 0:
                    loads[c].wait()
            else:
                before = hop(c, s - 1, way)
                before.wait_recv()
                before.wait_send()
            hop(c, s, way).start()

    def arrived(c):
        for way in range(2):
            last = hop(c, half_way, way)
            last.wait_recv()
            last.wait_send()

    def spread(source, target, send, recv):
        def copy(dr, dt, ahead):
            if ahead:
                span = pl.ds(pl.multiple_of(lax.rem(rep + reps - dr, reps) * rows, rows), rows)
                src = target.at[span, own_cols]
            else:
                span, src = own_rows, source
            step_r = 0 if ahead else dr
            return pltpu.make_async_remote_copy(
                src_ref=src,
                dst_ref=target.at[span, own_cols],
                send_sem=send.at[dr, dt],
                recv_sem=recv.at[dr, dt],
                device_id={"rep": lax.rem(rep + step_r, reps), "tp": lax.rem(tp + dt, tps)},
                device_id_type=MESH,
            )

        first = [copy(dr, 0, False) for dr in range(1, reps)]
        near = [copy(0, dt, False) for dt in range(1, tps)]
        for one in first + near:
            one.start()

        def forward():
            later = []
            for dr in range(1, reps):
                first[dr - 1].wait_recv()
                for dt in range(1, tps):
                    one = copy(dr, dt, True)
                    one.start()
                    later.append(one)
            return later

        def finish(later):
            for one in near + later:
                one.wait_recv()
            for one in first + near + later:
                one.wait_send()

        return forward, finish

    def norm_all(source, gain):
        def one(i, carry):
            span = pl.ds(pl.multiple_of(i * 64, 64), 64)
            x = source[span, :].astype(jnp.float32)
            scale = lax.rsqrt(jnp.mean(x * x, axis=-1, keepdims=True) + EPS)
            normed[span, :] = (x * scale * gain[...]).astype(jnp.bfloat16)
            return carry

        lax.fori_loop(0, tokens // 64, one, 0)

    def seq_rows(i):
        return pl.ds(pl.multiple_of(i * LENGTH, LENGTH), LENGTH)

    def mixer_rows(i):
        x = normed[seq_rows(i), :]
        value = jnp.dot(x, weights[0], preferred_element_type=jnp.float32)
        gate = jnp.dot(x, weights[1], preferred_element_type=jnp.float32)
        padded[LEAD : LEAD + LENGTH, :] = value * jax.nn.sigmoid(gate)

        def column(j, sums):
            cols = pl.ds(pl.multiple_of(j * LANES, LANES), LANES)
            from_all = pl.multiple_of(tp * own_width + rep * width + j * LANES, LANES)
            kern = conv_kernel[:, pl.ds(from_all, LANES)]
            total = jnp.zeros((LENGTH, LANES), jnp.float32)
            for tap in range(taps):
                begin = LEAD - (taps - 1) + tap
                total = total + kern[tap : tap + 1, :] * padded[begin : begin + LENGTH, cols]
            filtered[seq_rows(i), cols] = total
            return sums[0] + total, sums[1] + total * total

        zero = jnp.zeros((LENGTH, LANES), jnp.float32)
        one, two = lax.fori_loop(0, width // LANES, column, (zero, zero))
        lane = lax.broadcasted_iota(jnp.int32, (LENGTH, LANES), 1)
        both = jnp.where(
            lane == 0,
            jnp.sum(one, axis=-1, keepdims=True),
            jnp.where(lane == 1, jnp.sum(two, axis=-1, keepdims=True), 0.0),
        )
        own_stats[:, seq_rows(i)] = both.T[0:8, :]

    def stat_copies():
        copies = []
        for dr in range(reps):
            for dt in range(tps):
                if dr or dt:
                    copies.append(
                        pltpu.make_async_remote_copy(
                            src_ref=own_stats,
                            dst_ref=peer_stats.at[dr * tps + dt],
                            send_sem=stat_send.at[dr, dt],
                            recv_sem=stat_recv.at[dr, dt],
                            device_id={
                                "rep": lax.rem(rep + dr, reps),
                                "tp": lax.rem(tp + dt, tps),
                            },
                            device_id_type=MESH,
                        )
                    )
        return copies

    def activate_rows(i, carry):
        total = own_stats[:, seq_rows(i)]
        for k in range(1, reps * tps):
            total = total + peer_stats[k, :, seq_rows(i)]
        turned = jnp.concatenate([total] * (LANES // 8), axis=0).T
        mean = turned[:, 0:1] / channels
        variance = turned[:, 1:2] / channels - mean * mean
        gain_at = pl.multiple_of(tp * own_width + rep * width, LANES)
        gain = chan_gain[:, pl.ds(gain_at, width)]
        x = (filtered[seq_rows(i), :] - mean) * lax.rsqrt(variance + EPS) * gain
        activated[seq_rows(i), :] = (x / (1.0 + jnp.exp(-x))).astype(jnp.bfloat16)
        return carry

    def share(order, o, left, pieces_of, parts, peers, send, recv):
        span = pl.ds(pl.multiple_of(o * block, block), block)

        def one(i, carry):
            at = pl.ds(pl.multiple_of(i * rows, rows), rows)
            total = None
            for k, c in enumerate(pieces_of):
                term = times_transposed(
                    left[at, k * width : (k + 1) * width], weights[c, span, :]
                )
                total = term if total is None else total + term
            parts[o, at, :] = total.astype(jnp.bfloat16)
            return carry

        lax.fori_loop(0, reps, one, 0)
        keeper = o // per_tp
        dt = lax.rem(keeper + tps - tp, tps)
        waits = []
        for dr in [*range(1, reps), 0]:
            to = lax.rem(rep + dr, reps)
            copy = pltpu.make_async_remote_copy(
                src_ref=parts.at[o, pl.ds(pl.multiple_of(to * rows, rows), rows), :],
                dst_ref=peers.at[dr * tps + dt, lax.rem(o, per_tp)],
                send_sem=send.at[order, dr],
                recv_sem=recv.at[dr * tps + dt, lax.rem(o, per_tp)],
                device_id={"rep": to, "tp": keeper},
                device_id_type=MESH,
            )
            if dr:
                copy.start()
                waits.append(copy.wait_send)
            else:
                pl.when(keeper != tp)(copy.start)
                waits.append(lambda k=keeper, c=copy: pl.when(k != tp)(c.wait_send))
        return waits

    def wait_peers(j, parts, peers, send, recv):
        for k in range(1, reps * tps):
            dr, dt = k // tps, k % tps
            pltpu.make_async_remote_copy(
                src_ref=parts.at[0, own_rows, :],
                dst_ref=peers.at[k, j],
                send_sem=send.at[0, 0],
                recv_sem=recv.at[k, j],
                device_id={"rep": lax.rem(rep + dr, reps), "tp": lax.rem(tp + dt, tps)},
                device_id_type=MESH,
            ).wait_recv()

    def total_of(j, parts, peers):
        total = parts[tp * per_tp + j, own_rows, :].astype(jnp.float32)
        for k in range(1, reps * tps):
            total = total + peers[k, j].astype(jnp.float32)
        return total

    stepwise = blocks == n

    def owners(s):
        if s in (0, half_way):
            return [ring_index(place + s)]
        return [ring_index(place - s), ring_index(place + s)]

    def steps_of(c):
        return range(1, half_way + 1)

    first, second = (0, 1), (2, 3)
    third = tuple(range(4, 3 + ups))
    fourth = tuple(range(3 + ups, chunks))

    pump(0, 1)
    pump(1, 1)
    forward, finish = spread(states, rows_in, in_send, in_recv)
    padded[0:LEAD, :] = jnp.zeros((LEAD, width), jnp.float32)
    pump(0, 2)
    pump(1, 2)
    later = forward()
    for s in range(3, half_way + 1):
        pump(0, s)
        if s == 3:
            own_load.wait()
            finish(later)
        pump(1, s)
        if s == 3:
            norm_all(rows_in, mix_gain)
    pump(2, 1)
    pump(3, 1)
    arrived(0)
    arrived(1)

    todo = [(c, s) for s in range(2, half_way + 1) for c in second]

    def next_hop():
        if todo:
            pump(*todo.pop(0))

    for i in range(0, pieces, 2):
        lax.fori_loop(
            i, min(i + 2, pieces), lambda k, carry: (mixer_rows(k), carry)[1], 0
        )
        next_hop()
    stats = stat_copies()
    for one in stats:
        one.start()
    for one in stats:
        one.wait_recv()
    lax.fori_loop(0, pieces, activate_rows, 0)
    waits = []
    mix = (activated, (2,), mix_parts, mix_peers, mix_send, mix_recv)
    if stepwise:
        for s in range(half_way - 1):
            for o in owners(s):
                waits += share(len(waits) // reps, o, *mix)
    while todo:
        next_hop()
    if stepwise:
        for o in owners(half_way - 1):
            waits += share(len(waits) // reps, o, *mix)
    for c in third:
        pump(c, 1)
    arrived(2)
    if stepwise:
        waits += share(len(waits) // reps, owners(half_way)[0], *mix)
    else:
        for o in range(blocks):
            waits += share(o, o, *mix)

    todo = [(c, s) for s in range(2, half_way + 1) for c in third]
    for _ in range(len(todo) // 2):
        next_hop()
    for j in range(per_tp):
        wait_peers(j, mix_parts, mix_peers, mix_send, mix_recv)
        at = pl.ds(pl.multiple_of(tp * own_width + j * block, block), block)
        rows_mid[own_rows, at] = (
            rows_in[own_rows, at].astype(jnp.float32) + total_of(j, mix_parts, mix_peers)
        ).astype(jnp.bfloat16)
    forward, finish = spread(rows_mid.at[own_rows, own_cols], rows_mid, mid_send, mid_recv)
    while todo:
        next_hop()
    for c in fourth:
        pump(c, 1)
    arrived(3)
    for c in third:
        arrived(c)
    later = forward()
    finish(later)
    norm_all(rows_mid, mlp_gain)
    todo = [(c, s) for s in range(2, half_way + 1) for c in fourth]
    next_hop()
    for k in range(ups):

        def up_rows(i, carry):
            at = pl.ds(pl.multiple_of(i * rows, rows), rows)
            x = jnp.dot(normed[at, :], weights[3 + k], preferred_element_type=jnp.float32)
            x = jnp.maximum(x, 0.0)
            hidden[at, k * width : (k + 1) * width] = (x * x).astype(jnp.bfloat16)
            return carry

        lax.fori_loop(0, reps, up_rows, 0)
        next_hop()
    done = []
    fed = (hidden, fourth, fed_parts, fed_peers, fed_send, fed_recv)
    if stepwise:
        for o in owners(0):
            done += share(len(done) // reps, o, *fed)
    for s in range(2, half_way + 1):
        while todo and todo[0][1] <= s:
            next_hop()
        if stepwise:
            for o in owners(s - 1):
                done += share(len(done) // reps, o, *fed)
    for c in fourth:
        arrived(c)
    if stepwise:
        done += share(len(done) // reps, owners(half_way)[0], *fed)
    else:
        for o in range(blocks):
            done += share(o, o, *fed)
    for j in range(per_tp):
        wait_peers(j, fed_parts, fed_peers, fed_send, fed_recv)
        at = pl.ds(pl.multiple_of(tp * own_width + j * block, block), block)
        out[:, j * block : (j + 1) * block] = (
            rows_mid[own_rows, at].astype(jnp.float32) + total_of(j, fed_parts, fed_peers)
        ).astype(jnp.bfloat16)
    for one in stats:
        one.wait_send()
    for wait in waits + done:
        wait()


def body(mesh, states, mix_gain, w_value, w_gate, conv_kernel, chan_gain, w_mix, mlp_gain, w_up, w_down):
    reps, n, tps = mesh.shape["rep"], mesh.shape["fs"], mesh.shape["tp"]
    rows, own_width = states.shape
    width = own_width // reps
    channels = own_width * tps
    ups = w_up.shape[1] // own_width
    tokens = rows * reps
    group = reps * tps
    block = channels // n if channels // n >= LANES else own_width
    blocks, per_tp = channels // block, own_width // block
    chunks = 3 + 2 * ups
    bf16, f32 = jnp.bfloat16, jnp.float32
    vmem, hbm = pl.BlockSpec(memory_space=pltpu.VMEM), pl.BlockSpec(memory_space=pl.ANY)
    dma = pltpu.SemaphoreType.DMA
    return pl.pallas_call(
        functools.partial(kernel, (reps, n, tps, rows, channels, width, ups)),
        out_shape=jax.ShapeDtypeStruct((rows, own_width), bf16),
        in_specs=[hbm, vmem, hbm, hbm, vmem, vmem, hbm, vmem, hbm, hbm],
        out_specs=vmem,
        scratch_shapes=[
            pltpu.VMEM((chunks, channels, width), bf16),
            pltpu.VMEM((tokens, channels), bf16),
            pltpu.VMEM((tokens, channels), bf16),
            pltpu.VMEM((tokens, channels), bf16),
            pltpu.VMEM((LEAD + LENGTH, width), f32),
            pltpu.VMEM((tokens, width), f32),
            pltpu.VMEM((tokens, width), bf16),
            pltpu.VMEM((tokens, ups * width), bf16),
            pltpu.VMEM((8, tokens), f32),
            pltpu.VMEM((group, 8, tokens), f32),
            pltpu.VMEM((blocks, tokens, block), bf16),
            pltpu.VMEM((group, per_tp, rows, block), bf16),
            pltpu.VMEM((blocks, tokens, block), bf16),
            pltpu.VMEM((group, per_tp, rows, block), bf16),
            dma((chunks + 1,)),
            dma((2, chunks)),
            dma((2, chunks, n // 2)),
            dma((reps, tps)),
            dma((reps, tps)),
            dma((reps, tps)),
            dma((reps, tps)),
            dma((reps, tps)),
            dma((reps, tps)),
            dma((blocks, reps)),
            dma((group, per_tp)),
            dma((blocks, reps)),
            dma((group, per_tp)),
        ],
        compiler_params=pltpu.CompilerParams(
            collective_id=0, has_side_effects=True, vmem_limit_bytes=62 * 1024 * 1024
        ),
    )(
        states, mix_gain[None, :], w_value, w_gate, conv_kernel, chan_gain[None, :], w_mix,
        mlp_gain[None, :], w_up, w_down,
    )


def solution(mesh):
    in_specs = (
        P(("rep", "fs"), "tp"),
        P(),
        P("fs", "tp"),
        P("fs", "tp"),
        P(),
        P(),
        P("fs", "tp"),
        P(),
        P("fs", "tp"),
        P("fs", "tp"),
    )
    out_specs = P(("rep", "fs"), "tp")
    return jax.shard_map(
        functools.partial(body, mesh),
        mesh=mesh, in_specs=in_specs, out_specs=out_specs, check_vma=False,
    )
```

```python
import functools

import jax
import jax.numpy as jnp
from jax import lax
from jax.experimental import pallas as pl
from jax.experimental.pallas import tpu as pltpu
from jax.sharding import PartitionSpec as P

LENGTH = 128
LANES = 128
LEAD = 32
EPS = 1e-06
MESH = pl.DeviceIdType.MESH


def times_transposed(left, right):
    return lax.dot_general(
        left, right, (((1,), (1,)), ((), ())), preferred_element_type=jnp.float32
    )


def kernel(
    sizes,
    states, mix_gain, w_value, w_gate, conv_kernel, chan_gain, w_mix, mlp_gain, w_up, w_down,
    out,
    weights, rows_in, rows_mid, normed, padded, filtered, activated, hidden,
    own_stats, peer_stats, mix_parts, mix_peers, fed_parts, fed_peers,
    load_sems, ring_send, ring_recv, in_send, in_recv, mid_send, mid_recv,
    stat_send, stat_recv, mix_send, mix_recv, fed_send, fed_recv,
):
    reps, n, tps, rows, channels, width, ups = sizes
    own_width = width * reps
    half_way = n // 2
    shard = channels // n
    tokens = reps * rows
    pieces = tokens // LENGTH
    chunks = 3 + 2 * ups
    rep, fs, tp = lax.axis_index("rep"), lax.axis_index("fs"), lax.axis_index("tp")
    taps = conv_kernel.shape[0]
    blocks, _, block = mix_parts.shape
    per_tp = own_width // block

    def ring_index(place):
        place = lax.rem(place + n, n)
        return jnp.where(place < half_way, 2 * place, 2 * (n - 1 - place) + 1)

    place = jnp.where(lax.rem(fs, 2) == 0, fs // 2, n - 1 - fs // 2)
    neighbours = (ring_index(place + 1), ring_index(place - 1))

    barrier = pltpu.get_barrier_semaphore()
    for other in neighbours:
        pl.semaphore_signal(barrier, inc=1, device_id={"fs": other}, device_id_type=MESH)
    for dr in range(reps):
        for dt in range(tps):
            if dr or dt:
                pl.semaphore_signal(
                    barrier, inc=1,
                    device_id={"rep": lax.rem(rep + dr, reps), "tp": lax.rem(tp + dt, tps)},
                    device_id_type=MESH,
                )

    own_rows = pl.ds(pl.multiple_of(rep * rows, rows), rows)
    own_cols = pl.ds(pl.multiple_of(tp * own_width, own_width), own_width)

    def shard_at(owner, start=0, size=None):
        size = shard if size is None else size
        return pl.ds(pl.multiple_of(owner * shard + start, size), size)

    def hop(c, s, way):
        sign = 1 if way == 0 else -1
        owner = ring_index(place - sign * (s - 1))
        span = shard_at(owner)
        if s == half_way:
            span = shard_at(owner, way * (shard // 2), shard // 2)
        return pltpu.make_async_remote_copy(
            src_ref=weights.at[c, span, :],
            dst_ref=weights.at[c, span, :],
            send_sem=ring_send.at[way, c],
            recv_sem=ring_recv.at[way, c, s - 1],
            device_id={"fs": neighbours[way]},
            device_id_type=MESH,
        )

    loads = []
    for c in range(chunks):
        if c < 3:
            source, column = (w_value, w_gate, w_mix)[c], rep * width
        elif c < 3 + ups:
            source, column = w_up, (rep * ups + c - 3) * width
        else:
            source, column = w_down, (rep * ups + c - 3 - ups) * width
        loads.append(
            pltpu.make_async_copy(
                source.at[:, pl.ds(pl.multiple_of(column, width), width)],
                weights.at[c, shard_at(fs), :],
                load_sems.at[c],
            )
        )
        loads[-1].start()
    own_load = pltpu.make_async_copy(states, rows_in.at[own_rows, own_cols], load_sems.at[chunks])
    own_load.start()
    pl.semaphore_wait(barrier, 1 + reps * tps)

    def pump(c, s):
        for way in range(2):
            if s == 1:
                if way == 0:
                    loads[c].wait()
            else:
                before = hop(c, s - 1, way)
                before.wait_recv()
                before.wait_send()
            hop(c, s, way).start()

    def arrived(c):
        for way in range(2):
            last = hop(c, half_way, way)
            last.wait_recv()
            last.wait_send()

    def spread(source, target, send, recv):
        def copy(dr, dt, ahead):
            if ahead:
                span = pl.ds(pl.multiple_of(lax.rem(rep + reps - dr, reps) * rows, rows), rows)
                src = target.at[span, own_cols]
            else:
                span, src = own_rows, source
            step_r = 0 if ahead else dr
            return pltpu.make_async_remote_copy(
                src_ref=src,
                dst_ref=target.at[span, own_cols],
                send_sem=send.at[dr, dt],
                recv_sem=recv.at[dr, dt],
                device_id={"rep": lax.rem(rep + step_r, reps), "tp": lax.rem(tp + dt, tps)},
                device_id_type=MESH,
            )

        first = [copy(dr, 0, False) for dr in range(1, reps)]
        near = [copy(0, dt, False) for dt in range(1, tps)]
        for one in first + near:
            one.start()

        def forward():
            later = []
            for dr in range(1, reps):
                first[dr - 1].wait_recv()
                for dt in range(1, tps):
                    one = copy(dr, dt, True)
                    one.start()
                    later.append(one)
            return later

        def finish(later):
            for one in near + later:
                one.wait_recv()
            for one in first + near + later:
                one.wait_send()

        return forward, finish

    def norm_all(source, gain):
        def one(i, carry):
            span = pl.ds(pl.multiple_of(i * 64, 64), 64)
            x = source[span, :].astype(jnp.float32)
            scale = lax.rsqrt(jnp.mean(x * x, axis=-1, keepdims=True) + EPS)
            normed[span, :] = (x * scale * gain[...]).astype(jnp.bfloat16)
            return carry

        lax.fori_loop(0, tokens // 64, one, 0)

    def seq_rows(i):
        return pl.ds(pl.multiple_of(i * LENGTH, LENGTH), LENGTH)

    def mixer_rows(i):
        x = normed[seq_rows(i), :]
        value = jnp.dot(x, weights[0], preferred_element_type=jnp.float32)
        gate = jnp.dot(x, weights[1], preferred_element_type=jnp.float32)
        padded[LEAD : LEAD + LENGTH, :] = value * jax.nn.sigmoid(gate)

        def column(j, sums):
            cols = pl.ds(pl.multiple_of(j * LANES, LANES), LANES)
            from_all = pl.multiple_of(tp * own_width + rep * width + j * LANES, LANES)
            kern = conv_kernel[:, pl.ds(from_all, LANES)]
            total = jnp.zeros((LENGTH, LANES), jnp.float32)
            for tap in range(taps):
                begin = LEAD - (taps - 1) + tap
                total = total + kern[tap : tap + 1, :] * padded[begin : begin + LENGTH, cols]
            filtered[seq_rows(i), cols] = total
            return sums[0] + total, sums[1] + total * total

        zero = jnp.zeros((LENGTH, LANES), jnp.float32)
        one, two = lax.fori_loop(0, width // LANES, column, (zero, zero))
        lane = lax.broadcasted_iota(jnp.int32, (LENGTH, LANES), 1)
        both = jnp.where(
            lane == 0,
            jnp.sum(one, axis=-1, keepdims=True),
            jnp.where(lane == 1, jnp.sum(two, axis=-1, keepdims=True), 0.0),
        )
        own_stats[:, seq_rows(i)] = both.T[0:8, :]

    def stat_copies():
        copies = []
        for dr in range(reps):
            for dt in range(tps):
                if dr or dt:
                    copies.append(
                        pltpu.make_async_remote_copy(
                            src_ref=own_stats,
                            dst_ref=peer_stats.at[dr * tps + dt],
                            send_sem=stat_send.at[dr, dt],
                            recv_sem=stat_recv.at[dr, dt],
                            device_id={
                                "rep": lax.rem(rep + dr, reps),
                                "tp": lax.rem(tp + dt, tps),
                            },
                            device_id_type=MESH,
                        )
                    )
        return copies

    def activate_rows(i, carry):
        total = own_stats[:, seq_rows(i)]
        for k in range(1, reps * tps):
            total = total + peer_stats[k, :, seq_rows(i)]
        turned = jnp.concatenate([total] * (LANES // 8), axis=0).T
        mean = turned[:, 0:1] / channels
        variance = turned[:, 1:2] / channels - mean * mean
        gain_at = pl.multiple_of(tp * own_width + rep * width, LANES)
        gain = chan_gain[:, pl.ds(gain_at, width)]
        x = (filtered[seq_rows(i), :] - mean) * lax.rsqrt(variance + EPS) * gain
        activated[seq_rows(i), :] = (x / (1.0 + jnp.exp(-x))).astype(jnp.bfloat16)
        return carry

    def share(order, o, left, pieces_of, parts, peers, send, recv):
        span = pl.ds(pl.multiple_of(o * block, block), block)

        def one(i):
            at = pl.ds(pl.multiple_of(i * rows, rows), rows)
            total = None
            for k, c in enumerate(pieces_of):
                term = times_transposed(
                    left[at, k * width : (k + 1) * width], weights[c, span, :]
                )
                total = term if total is None else total + term
            parts[o, at, :] = total.astype(jnp.bfloat16)

        keeper = o // per_tp
        dt = lax.rem(keeper + tps - tp, tps)
        waits = []
        for dr in [*range(1, reps), 0]:
            to = lax.rem(rep + dr, reps)
            one(to)
            copy = pltpu.make_async_remote_copy(
                src_ref=parts.at[o, pl.ds(pl.multiple_of(to * rows, rows), rows), :],
                dst_ref=peers.at[dr * tps + dt, lax.rem(o, per_tp)],
                send_sem=send.at[order, dr],
                recv_sem=recv.at[dr * tps + dt, lax.rem(o, per_tp)],
                device_id={"rep": to, "tp": keeper},
                device_id_type=MESH,
            )
            if dr:
                copy.start()
                waits.append(copy.wait_send)
            else:
                pl.when(keeper != tp)(copy.start)
                waits.append(lambda k=keeper, c=copy: pl.when(k != tp)(c.wait_send))
        return waits

    def wait_peers(j, parts, peers, send, recv):
        for k in range(1, reps * tps):
            dr, dt = k // tps, k % tps
            pltpu.make_async_remote_copy(
                src_ref=parts.at[0, own_rows, :],
                dst_ref=peers.at[k, j],
                send_sem=send.at[0, 0],
                recv_sem=recv.at[k, j],
                device_id={"rep": lax.rem(rep + dr, reps), "tp": lax.rem(tp + dt, tps)},
                device_id_type=MESH,
            ).wait_recv()

    def total_of(j, parts, peers):
        total = parts[tp * per_tp + j, own_rows, :].astype(jnp.float32)
        for k in range(1, reps * tps):
            total = total + peers[k, j].astype(jnp.float32)
        return total

    stepwise = blocks == n

    def owners(s):
        if s in (0, half_way):
            return [ring_index(place + s)]
        return [ring_index(place - s), ring_index(place + s)]

    def steps_of(c):
        return range(1, half_way + 1)

    first, second = (0, 1), (2, 3)
    third = tuple(range(4, 3 + ups))
    fourth = tuple(range(3 + ups, chunks))

    pump(0, 1)
    pump(1, 1)
    forward, finish = spread(states, rows_in, in_send, in_recv)
    padded[0:LEAD, :] = jnp.zeros((LEAD, width), jnp.float32)
    pump(0, 2)
    pump(1, 2)
    later = forward()
    for s in range(3, half_way + 1):
        pump(0, s)
        if s == 3:
            own_load.wait()
            finish(later)
        pump(1, s)
        if s == 3:
            norm_all(rows_in, mix_gain)
    pump(2, 1)
    pump(3, 1)
    arrived(0)
    arrived(1)

    todo = [(c, s) for s in range(2, half_way + 1) for c in second]

    def next_hop():
        if todo:
            pump(*todo.pop(0))

    for i in range(0, pieces, 2):
        lax.fori_loop(
            i, min(i + 2, pieces), lambda k, carry: (mixer_rows(k), carry)[1], 0
        )
        next_hop()
    stats = stat_copies()
    for one in stats:
        one.start()
    for one in stats:
        one.wait_recv()
    lax.fori_loop(0, pieces, activate_rows, 0)
    waits = []
    mix = (activated, (2,), mix_parts, mix_peers, mix_send, mix_recv)
    if stepwise:
        for s in range(half_way - 1):
            for o in owners(s):
                waits += share(len(waits) // reps, o, *mix)
    while todo:
        next_hop()
    if stepwise:
        for o in owners(half_way - 1):
            waits += share(len(waits) // reps, o, *mix)
    for c in third:
        pump(c, 1)
    arrived(2)
    if stepwise:
        waits += share(len(waits) // reps, owners(half_way)[0], *mix)
    else:
        for o in range(blocks):
            waits += share(o, o, *mix)

    todo = [(c, s) for s in range(2, half_way + 1) for c in third]
    for _ in range(len(todo) // 2):
        next_hop()
    for j in range(per_tp):
        wait_peers(j, mix_parts, mix_peers, mix_send, mix_recv)
        at = pl.ds(pl.multiple_of(tp * own_width + j * block, block), block)
        rows_mid[own_rows, at] = (
            rows_in[own_rows, at].astype(jnp.float32) + total_of(j, mix_parts, mix_peers)
        ).astype(jnp.bfloat16)
    forward, finish = spread(rows_mid.at[own_rows, own_cols], rows_mid, mid_send, mid_recv)
    while todo:
        next_hop()
    for c in fourth:
        pump(c, 1)
    arrived(3)
    for c in third:
        arrived(c)
    later = forward()
    finish(later)
    norm_all(rows_mid, mlp_gain)
    todo = [(c, s) for s in range(2, half_way + 1) for c in fourth]
    next_hop()
    for k in range(ups):

        def up_rows(i, carry):
            at = pl.ds(pl.multiple_of(i * rows, rows), rows)
            x = jnp.dot(normed[at, :], weights[3 + k], preferred_element_type=jnp.float32)
            x = jnp.maximum(x, 0.0)
            hidden[at, k * width : (k + 1) * width] = (x * x).astype(jnp.bfloat16)
            return carry

        lax.fori_loop(0, reps, up_rows, 0)
        next_hop()
    done = []
    fed = (hidden, fourth, fed_parts, fed_peers, fed_send, fed_recv)
    if stepwise:
        for o in owners(0):
            done += share(len(done) // reps, o, *fed)
    for s in range(2, half_way + 1):
        while todo and todo[0][1] <= s:
            next_hop()
        if stepwise:
            for o in owners(s - 1):
                done += share(len(done) // reps, o, *fed)
    for c in fourth:
        arrived(c)
    if stepwise:
        done += share(len(done) // reps, owners(half_way)[0], *fed)
    else:
        for o in range(blocks):
            done += share(o, o, *fed)
    for j in range(per_tp):
        wait_peers(j, fed_parts, fed_peers, fed_send, fed_recv)
        at = pl.ds(pl.multiple_of(tp * own_width + j * block, block), block)
        out[:, j * block : (j + 1) * block] = (
            rows_mid[own_rows, at].astype(jnp.float32) + total_of(j, fed_parts, fed_peers)
        ).astype(jnp.bfloat16)
    for one in stats:
        one.wait_send()
    for wait in waits + done:
        wait()


def body(mesh, states, mix_gain, w_value, w_gate, conv_kernel, chan_gain, w_mix, mlp_gain, w_up, w_down):
    reps, n, tps = mesh.shape["rep"], mesh.shape["fs"], mesh.shape["tp"]
    rows, own_width = states.shape
    width = own_width // reps
    channels = own_width * tps
    ups = w_up.shape[1] // own_width
    tokens = rows * reps
    group = reps * tps
    block = channels // n if channels // n >= LANES else own_width
    blocks, per_tp = channels // block, own_width // block
    chunks = 3 + 2 * ups
    bf16, f32 = jnp.bfloat16, jnp.float32
    vmem, hbm = pl.BlockSpec(memory_space=pltpu.VMEM), pl.BlockSpec(memory_space=pl.ANY)
    dma = pltpu.SemaphoreType.DMA
    return pl.pallas_call(
        functools.partial(kernel, (reps, n, tps, rows, channels, width, ups)),
        out_shape=jax.ShapeDtypeStruct((rows, own_width), bf16),
        in_specs=[hbm, vmem, hbm, hbm, vmem, vmem, hbm, vmem, hbm, hbm],
        out_specs=vmem,
        scratch_shapes=[
            pltpu.VMEM((chunks, channels, width), bf16),
            pltpu.VMEM((tokens, channels), bf16),
            pltpu.VMEM((tokens, channels), bf16),
            pltpu.VMEM((tokens, channels), bf16),
            pltpu.VMEM((LEAD + LENGTH, width), f32),
            pltpu.VMEM((tokens, width), f32),
            pltpu.VMEM((tokens, width), bf16),
            pltpu.VMEM((tokens, ups * width), bf16),
            pltpu.VMEM((8, tokens), f32),
            pltpu.VMEM((group, 8, tokens), f32),
            pltpu.VMEM((blocks, tokens, block), bf16),
            pltpu.VMEM((group, per_tp, rows, block), bf16),
            pltpu.VMEM((blocks, tokens, block), bf16),
            pltpu.VMEM((group, per_tp, rows, block), bf16),
            dma((chunks + 1,)),
            dma((2, chunks)),
            dma((2, chunks, n // 2)),
            dma((reps, tps)),
            dma((reps, tps)),
            dma((reps, tps)),
            dma((reps, tps)),
            dma((reps, tps)),
            dma((reps, tps)),
            dma((blocks, reps)),
            dma((group, per_tp)),
            dma((blocks, reps)),
            dma((group, per_tp)),
        ],
        compiler_params=pltpu.CompilerParams(
            collective_id=0, has_side_effects=True, vmem_limit_bytes=62 * 1024 * 1024
        ),
    )(
        states, mix_gain[None, :], w_value, w_gate, conv_kernel, chan_gain[None, :], w_mix,
        mlp_gain[None, :], w_up, w_down,
    )


def solution(mesh):
    in_specs = (
        P(("rep", "fs"), "tp"),
        P(),
        P("fs", "tp"),
        P("fs", "tp"),
        P(),
        P(),
        P("fs", "tp"),
        P(),
        P("fs", "tp"),
        P("fs", "tp"),
    )
    out_specs = P(("rep", "fs"), "tp")
    return jax.shard_map(
        functools.partial(body, mesh),
        mesh=mesh, in_specs=in_specs, out_specs=out_specs, check_vma=False,
    )
```
